256 devices in a mesh: ep: 64 (over z, x, core), tp: 4 (over y).
Axes of the slice: x: 4, y: 4, z: 8, core: 2. Of those that a mesh axis runs over, the one named last changes fastest.
Arguments:
- query_latent: bfloat16 [8192, 512], P('ep'), may hold values from -6 to 6
- key_latent: bfloat16 [8192, 256], P('ep'), may hold values from -6 to 6
- rope_key: bfloat16 [8192, 64], P('ep'), may hold values from -500 to 500
- query_gain: float32 [512], replicated, may hold values from 0.1 to 1.9
- key_gain: float32 [256], replicated, may hold values from 0.1 to 1.9
- w_query: bfloat16 [512, 1024], P(None, 'tp'), may hold values from -0.25 to 0.25
- w_query_rope: bfloat16 [512, 512], P(None, 'tp'), may hold values from -0.25 to 0.25
- w_key: bfloat16 [256, 1024], P(None, 'tp'), may hold values from -0.375 to 0.375
- w_value: bfloat16 [256, 1024], P(None, 'tp'), may hold values from -0.375 to 0.375
- w_out: bfloat16 [1024, 2048], P('tp'), may hold values from -1.796875 to 1.796875
- tokens_b: bfloat16 [32768, 2048], P('ep'), may hold values from -6 to 6
- ffn_gain: float32 [2048], replicated, may hold values from 0.1 to 1.9
- route_expert: int32 [32768, 2], P('ep'), may hold values from 0 to 63, as said below
- route_weight: float32 [32768, 2], P('ep'), may hold values from 0.2 to 1
- w_gate: bfloat16 [64, 2048, 1024], P('ep', None, 'tp'), may hold values from -0.125 to 0.125
- w_up: bfloat16 [64, 2048, 1024], P('ep', None, 'tp'), may hold values from -0.125 to 0.125
- w_down: bfloat16 [64, 1024, 2048], P('ep', 'tp'), may hold values from -0.1875 to 0.1875
Outputs:
- mixer_out: bfloat16 [8192, 2048], P(('ep', 'tp'))
- moe_out: bfloat16 [32768, 2048], P('ep', 'tp')
The draws below stay inside these ranges and needn't reach their ends.
Inputs may be any that keep to these rules, and one draw needn't show every extreme that they name: `route_expert`: expert e belongs to group e // 16. A row's 2 experts differ and lie in one group. Among the rows of one device along ep, every group is named by exactly 128 rows and every expert is named exactly 16 times.
All inputs are finite; a program needn't handle non-finite values.
Results may differ from the reference program's by a relative error of at most 0.013.
The reference program's roundings to bfloat16 on the way count: a program that leaves them out, or rounds other values in their place, can miss the bound.
Values may be sent and summed in bfloat16 or wider, within the bound.
No kernel may reach another device: no remote copies, remote signals or barrier semaphores. Data moves between devices by JAX's collectives and lax.ppermute only.
A program may use at most 64 MiB of HBM per device.

```python
import math
import jax
import jax.numpy as jnp
from jax import lax

D = 2048
HEADS = 8
NOPE = 128
ROPE = 64
VDIM = 128
QRANK = 512
KVRANK = 256
GRID_W = 64
FF_E = 1024
GROUPS = 4
TOPK = 2
TOK_A = 128
TOK_B = 512
EXPERTS = 64
TOKENS_A = 8192
TOKENS_B = 32768
N_EP = 64
N_TP = 4


def draw_rope_key(key, part):
    seq_len = TOK_A * N_EP
    key_base = jax.random.fold_in(key, 0)
    return jnp.clip(3.0 * jax.random.normal(key_base, (seq_len, ROPE), jnp.float32), -18.0, 18.0).astype(jnp.bfloat16)


def draw_route_expert(key, part):
    group_rows = TOK_B // GROUPS
    in_group = EXPERTS // GROUPS
    key_order, key_rotation, key_shift = jax.random.split(key, 3)
    ranking = jax.random.randint(key_order, (N_EP, TOK_B), 0, 1 << 16) * TOK_B + jnp.arange(TOK_B, dtype=jnp.int32)[None, :]
    ordering = jnp.argsort(ranking, axis=1, stable=True)
    position = jnp.argsort(ordering, axis=1, stable=True).astype(jnp.int32)
    group_of = position // group_rows
    within = position % group_rows
    rotation = jax.random.randint(key_rotation, (N_EP, GROUPS), 0, in_group)
    shifted = jax.random.randint(key_shift, (N_EP, GROUPS), 1, in_group)
    rotation_row = jnp.take_along_axis(rotation, group_of, axis=1)
    shift_row = jnp.take_along_axis(shifted, group_of, axis=1)
    first_choice = group_of * in_group + (within + rotation_row) % in_group
    second_choice = group_of * in_group + (within + rotation_row + shift_row) % in_group
    routes = jnp.stack([first_choice, second_choice], axis=-1)
    return routes.reshape(N_EP * TOK_B, TOPK).astype(jnp.int32)


def levels(key, extent, pieces, smallest, top_value):
    loudness = 1.0
    for dim, shards_of in pieces:
        draws = jax.random.uniform(jax.random.fold_in(jax.random.fold_in(key, 6), dim), (shards_of,), jnp.float32, smallest / len(pieces), top_value / len(pieces))
        loudness = loudness * jnp.repeat(jnp.exp(draws), extent[dim] // shards_of).reshape((-1,) + (1,) * (len(extent) - 1 - dim))
    return loudness


def noise(stream_key, shape, deviation, most, cuts=(), held_as=jnp.bfloat16):
    values = jax.random.normal(stream_key, shape, jnp.float32) * deviation
    if len(cuts) > 0:
        values = levels(stream_key, shape, cuts, -0.22, 0.18) * values
    return jnp.clip(values, min=-most, max=most).astype(held_as)


def setup_inputs(seed: int = 0) -> dict:
    key_of = jax.random.split(jax.random.key(seed), 18)
    query_latent = noise(key_of[0], (TOKENS_A, QRANK), 1.0, 6.0, ((0, 64),))
    key_latent = noise(key_of[1], (TOKENS_A, KVRANK), 1.0, 6.0, ((0, 64),))
    rope_key = draw_rope_key(jax.random.fold_in(key_of[17], 71), 0)
    query_gain = jnp.clip(1.0 + 0.18 * jax.random.normal(key_of[3], (QRANK,), jnp.float32), 0.1, 1.9)
    key_gain = jnp.clip(1.0 + 0.18 * jax.random.normal(key_of[4], (KVRANK,), jnp.float32), 0.1, 1.9)
    w_query = noise(key_of[5], (QRANK, HEADS * NOPE), QRANK ** -0.5, 0.25, ((1, 4),))
    w_query_rope = noise(key_of[6], (QRANK, HEADS * ROPE), QRANK ** -0.5, 0.25, ((1, 4),))
    w_key = noise(key_of[7], (KVRANK, HEADS * NOPE), KVRANK ** -0.5, 0.375, ((1, 4),))
    w_value = noise(key_of[8], (KVRANK, HEADS * VDIM), KVRANK ** -0.5, 0.375, ((1, 4),))
    w_out = noise(key_of[9], (HEADS * VDIM, D), 0.3, 1.796875, ((0, 4),))
    tokens_b = noise(key_of[10], (TOKENS_B, D), 1.0, 6.0, ((0, 64),))
    ffn_gain = jnp.clip(1.0 + 0.18 * jax.random.normal(key_of[11], (D,), jnp.float32), 0.1, 1.9)
    route_expert = draw_route_expert(jax.random.fold_in(key_of[17], 71), 0)
    route_weight = jnp.clip(jnp.exp(math.log(1.0) - 1.609438 * jax.random.uniform(key_of[13], (TOKENS_B, TOPK), jnp.float32) ** levels(key_of[13], (TOKENS_B, TOPK), ((0, 64),), -0.2, 0.2)), 0.2, 1.0)
    w_gate = noise(key_of[14], (EXPERTS, D, FF_E), D ** -0.5, 0.125, ((0, 64), (2, 4)))
    w_up = noise(key_of[15], (EXPERTS, D, FF_E), D ** -0.5, 0.125, ((0, 64), (2, 4)))
    w_down = noise(key_of[16], (EXPERTS, FF_E, D), FF_E ** -0.5, 0.1875, ((0, 64), (1, 4)))
    return {"query_latent": query_latent, "key_latent": key_latent, "rope_key": rope_key, "query_gain": query_gain, "key_gain": key_gain, "w_query": w_query, "w_query_rope": w_query_rope, "w_key": w_key, "w_value": w_value, "w_out": w_out, "tokens_b": tokens_b, "ffn_gain": ffn_gain, "route_expert": route_expert, "route_weight": route_weight, "w_gate": w_gate, "w_up": w_up, "w_down": w_down}


epsilon = 1e-06
rotary_base = 10000.0

def rms_scale(values_in, gain):
    widened = values_in.astype(jnp.float32)
    normed = widened * lax.rsqrt(lax.optimization_barrier(jnp.mean(widened * widened, axis=-1, keepdims=True)) + epsilon)
    return (normed * gain.astype(jnp.float32)).astype(jnp.bfloat16)

def rotary_tables(positions):
    half_width = ROPE // 2
    inverse = rotary_base ** (-jnp.arange(0, half_width, 2, dtype=jnp.float32) / half_width)
    grid_row = (positions // GRID_W).astype(jnp.float32)
    grid_col = (positions % GRID_W).astype(jnp.float32)
    angle = jnp.concatenate([grid_row[:, None] * inverse, grid_col[:, None] * inverse], axis=-1)
    return (jnp.cos(angle), jnp.sin(angle))

def rotate(values_in, cosine, sine):
    even_part = values_in[..., 0::2]
    odd_part = values_in[..., 1::2]
    turned = jnp.stack([even_part * cosine - odd_part * sine, even_part * sine + odd_part * cosine], axis=-1)
    return turned.reshape(values_in.shape)

def mixer_half(query_latent, key_latent, rope_key, query_gain, key_gain, w_query, w_query_rope, w_key, w_value, w_out):
    seq_len = query_latent.shape[0]
    positions = jnp.arange(seq_len, dtype=jnp.int32)
    cosine, sine = rotary_tables(positions)
    query_normed = rms_scale(query_latent, query_gain)
    query_nope = jnp.dot(query_normed, w_query, preferred_element_type=jnp.float32).astype(jnp.bfloat16)
    query_nope = query_nope.reshape(seq_len, HEADS, NOPE)
    query_rot = jnp.dot(query_normed, w_query_rope, preferred_element_type=jnp.float32).reshape(seq_len, HEADS, ROPE)
    query_rot = rotate(query_rot, cosine[:, None, :], sine[:, None, :]).astype(jnp.bfloat16)
    key_normed = rms_scale(key_latent, key_gain)
    key_nope = jnp.dot(key_normed, w_key, preferred_element_type=jnp.float32).astype(jnp.bfloat16)
    key_nope = key_nope.reshape(seq_len, HEADS, NOPE)
    value_rows = jnp.dot(key_normed, w_value, preferred_element_type=jnp.float32).astype(jnp.bfloat16)
    value_rows = value_rows.reshape(seq_len, HEADS, VDIM)
    key_rot = rotate(rope_key.astype(jnp.float32), cosine, sine).astype(jnp.bfloat16)
    score_scale = (NOPE + ROPE) ** (-0.5)
    block_rows = math.gcd(seq_len, 512)

    def one_head(operands):
        head_query, head_rot, head_key, head_value = operands

        def one_block(block_operands):
            block_query, block_rot = block_operands
            scores = jnp.dot(block_query, head_key.T, preferred_element_type=jnp.float32)
            scores = (scores + jnp.dot(block_rot, key_rot.T, preferred_element_type=jnp.float32)) * score_scale
            row_max = lax.optimization_barrier(jnp.max(scores, axis=-1, keepdims=True))
            weights = jnp.exp(scores - row_max)
            totals = lax.optimization_barrier(jnp.sum(weights, axis=-1, keepdims=True))
            mixed = jnp.dot(weights.astype(jnp.bfloat16), head_value, preferred_element_type=jnp.float32)
            return (mixed / totals).astype(jnp.bfloat16)
        blocks = lax.map(one_block, (head_query.reshape(seq_len // block_rows, block_rows, NOPE), head_rot.reshape(seq_len // block_rows, block_rows, ROPE)))
        return blocks.reshape(seq_len, VDIM)
    heads_out = lax.map(one_head, (jnp.moveaxis(query_nope, 1, 0), jnp.moveaxis(query_rot, 1, 0), jnp.moveaxis(key_nope, 1, 0), jnp.moveaxis(value_rows, 1, 0)))
    heads_flat = jnp.moveaxis(heads_out, 0, 1).reshape(seq_len, HEADS * VDIM)
    group_cols = HEADS * VDIM // N_TP
    summed = jnp.zeros((seq_len, D), jnp.float32)
    for group_index in range(N_TP):
        lower = group_index * group_cols
        piece_sum = jnp.dot(heads_flat[:, lower:lower + group_cols], w_out[lower:lower + group_cols], preferred_element_type=jnp.float32).astype(jnp.bfloat16)
        summed = summed + lax.optimization_barrier(piece_sum).astype(jnp.float32)
    return summed.astype(jnp.bfloat16)

def expert_half(tokens_b, ffn_gain, route_expert, route_weight, w_gate, w_up, w_down):
    all_rows = tokens_b.shape[0]
    capacity = TOPK * TOK_B // EXPERTS
    normed = rms_scale(tokens_b, ffn_gain)
    copies = route_expert.reshape(N_EP, TOK_B * TOPK)
    expert_ids = jnp.arange(EXPERTS, dtype=jnp.int32)

    def block_slots(block_copies):
        chosen = (block_copies[:, None] == expert_ids[None, :]).astype(jnp.int32)
        earlier = jnp.cumsum(chosen, axis=0) - chosen
        return lax.optimization_barrier(jnp.sum(earlier * chosen, axis=1)).astype(jnp.int32)
    slot_index = lax.map(block_slots, copies)
    block_ids = jnp.arange(N_EP, dtype=jnp.int32)[:, None]
    target = (copies * (N_EP * capacity) + block_ids * capacity + slot_index).reshape(-1).astype(jnp.int32)
    source_row = jnp.zeros((EXPERTS * N_EP * capacity,), jnp.int32).at[target].set(jnp.arange(all_rows * TOPK, dtype=jnp.int32) // TOPK)
    source_row = source_row.reshape(EXPERTS, N_EP * capacity)
    unit_cols = FF_E // N_TP

    def one_expert(operands):
        row_ids, gate_weight, up_weight, down_weight = operands
        arrived = jnp.take(normed, row_ids, axis=0)
        gate_act = jnp.dot(arrived, gate_weight, preferred_element_type=jnp.float32)
        up_act = jnp.dot(arrived, up_weight, preferred_element_type=jnp.float32)
        hidden = (jax.nn.silu(gate_act) * up_act).astype(jnp.bfloat16)
        summed = jnp.zeros((arrived.shape[0], D), jnp.float32)
        for group_index in range(N_TP):
            lower = group_index * unit_cols
            piece_sum = jnp.dot(hidden[:, lower:lower + unit_cols], down_weight[lower:lower + unit_cols], preferred_element_type=jnp.float32).astype(jnp.bfloat16)
            summed = summed + lax.optimization_barrier(piece_sum).astype(jnp.float32)
        return summed.astype(jnp.bfloat16)
    results = lax.map(one_expert, (source_row, w_gate, w_up, w_down)).reshape(EXPERTS * N_EP * capacity, D)
    picked = jnp.take(results, target, axis=0).reshape(all_rows, TOPK, D)
    combined = lax.optimization_barrier(jnp.sum(picked.astype(jnp.float32) * route_weight[:, :, None], axis=1))
    return combined.astype(jnp.bfloat16)

def reference(query_latent, key_latent, rope_key, query_gain, key_gain, w_query, w_query_rope, w_key, w_value, w_out, tokens_b, ffn_gain, route_expert, route_weight, w_gate, w_up, w_down):
    mixer_out = mixer_half(query_latent, key_latent, rope_key, query_gain, key_gain, w_query, w_query_rope, w_key, w_value, w_out)
    moe_out = expert_half(tokens_b, ffn_gain, route_expert, route_weight, w_gate, w_up, w_down)
    return (mixer_out, moe_out)
```

```python
import functools
import math

import jax
import jax.numpy as jnp
import numpy as np
from jax import lax
from jax.experimental import pallas as pl
from jax.experimental.pallas import tpu as pltpu
from jax.sharding import PartitionSpec as P

NOPE = 128
ROPE = 64
VDIM = 128
GRID_W = 64
TOPK = 2
CHUNKS = 2

epsilon = 1e-06
rotary_base = 10000.0
neg_large = -1e30
f32 = jnp.float32
bf16 = jnp.bfloat16


def whole(shape):
    return pl.BlockSpec(shape, lambda *_: (0,) * len(shape))


def params(mib):
    return pltpu.CompilerParams(vmem_limit_bytes=mib * 1024 * 1024)


def dot_t(a, b):
    return lax.dot_general(a, b, (((1,), (1,)), ((), ())), preferred_element_type=f32)


def dot_0(a, b):
    return lax.dot_general(a, b, (((0,), (0,)), ((), ())), preferred_element_type=f32)


def dot(a, b):
    return jnp.dot(a, b, preferred_element_type=f32)


def iota(shape, dim):
    return lax.broadcasted_iota(jnp.int32, shape, dim)


def rms(widened, gain):
    normed = widened * lax.rsqrt(jnp.mean(widened * widened, axis=-1, keepdims=True) + epsilon)
    return (normed * gain).astype(bf16)


def swap_matrix(n):
    row, col = iota((n, n), 0), iota((n, n), 1)
    minus = (row == col + 1) & (col % 2 == 0)
    plus = (row + 1 == col) & (col % 2 == 1)
    return (jnp.where(plus, 1.0, 0.0) - jnp.where(minus, 1.0, 0.0)).astype(bf16)


def latent_kernel(kl_ref, rk_ref, kg_ref, cos_ref, sin_ref, send_ref):
    normed = rms(kl_ref[...].astype(f32), kg_ref[...])
    turned = rk_ref[...].astype(f32) * cos_ref[...] + dot(rk_ref[...], swap_matrix(ROPE)) * sin_ref[...]
    rank = kl_ref.shape[1]
    send_ref[:, :rank] = normed
    send_ref[:, rank:] = jnp.concatenate([turned.astype(bf16), jnp.zeros(turned.shape, bf16)], axis=1)


def query_kernel(ql_ref, qg_ref, wq_ref, wqr_ref, cos_ref, sin_ref, q_ref):
    heads = q_ref.shape[0]
    normed = rms(ql_ref[...].astype(f32), qg_ref[...])
    nope = dot(normed, wq_ref[...]).astype(bf16)
    swapped = dot(wqr_ref[...], swap_matrix(heads * ROPE)).astype(bf16)
    plain = dot(normed, wqr_ref[...])
    other = dot(normed, swapped)
    for h in range(heads):
        at = slice(h * ROPE, (h + 1) * ROPE)
        rot = (plain[:, at] * cos_ref[...] + other[:, at] * sin_ref[...]).astype(bf16)
        q_ref[h] = jnp.concatenate([nope[:, h * NOPE : (h + 1) * NOPE], rot, jnp.zeros(rot.shape, bf16)], axis=1)


def attend_kernel(me_ref, q_ref, kv_ref, wk_ref, wv_ref, wo_ref, *rest):
    out_refs, (all_ref, m_ref, l_ref, acc_ref) = rest[:-4], rest[-4:]
    heads, tok_rows = q_ref.shape[:2]
    rank = wk_ref.shape[0]
    scale = (NOPE + ROPE) ** (-0.5)

    @pl.when(pl.program_id(0) == 0)
    def _():
        m_ref[...] = jnp.full(m_ref.shape, neg_large, f32)
        l_ref[...] = jnp.zeros(l_ref.shape, f32)
        acc_ref[...] = jnp.zeros(acc_ref.shape, f32)

    latent = kv_ref[:, :rank]
    turned = kv_ref[:, rank:]
    keys = dot(latent, wk_ref[...]).astype(bf16)
    values = dot(latent, wv_ref[...]).astype(bf16)
    for h in range(heads):
        both = jnp.concatenate([keys[:, h * NOPE : (h + 1) * NOPE], turned], axis=1)
        scores = dot_t(both, q_ref[h]) * scale
        old = m_ref[h : h + 1, :]
        new = jnp.maximum(old, jnp.max(scores, axis=0, keepdims=True))
        weights = jnp.exp(scores - new)
        shrink = jnp.exp(old - new)
        m_ref[h : h + 1, :] = new
        l_ref[h : h + 1, :] = l_ref[h : h + 1, :] * shrink + jnp.sum(weights, axis=0, keepdims=True)
        added = dot_0(values[:, h * VDIM : (h + 1) * VDIM], weights.astype(bf16))
        acc_ref[h] = acc_ref[h] * shrink + added

    @pl.when(pl.program_id(0) == pl.num_programs(0) - 1)
    def _():
        parts = [(acc_ref[h] / l_ref[h : h + 1, :]).astype(bf16) for h in range(heads)]
        all_ref[...] = dot_0(jnp.concatenate(parts, axis=0), wo_ref[...]).astype(bf16)
        share = tok_rows // len(out_refs)
        for k, out_ref in enumerate(out_refs):
            owner = lax.rem(me_ref[0] + k, len(out_refs))
            out_ref[...] = all_ref[pl.ds(pl.multiple_of(owner * share, share), share), :]


def rotary_lanes(tok_rows):
    positions = lax.axis_index("ep") * tok_rows + jnp.arange(tok_rows, dtype=jnp.int32)
    half = ROPE // 2
    inverse = rotary_base ** (-np.arange(0, half, 2, dtype=np.float32) / half)
    pair = np.arange(ROPE) // 2
    spread = jnp.asarray(inverse.astype(np.float32)[pair % (half // 2)])
    by_row = jnp.asarray(pair < half // 2)
    grid_row = (positions // GRID_W).astype(f32)
    grid_col = (positions % GRID_W).astype(f32)
    angle = jnp.where(by_row[None, :], grid_row[:, None], grid_col[:, None]) * spread[None, :]
    return jnp.cos(angle), jnp.sin(angle)


def prep_kernel(me_ref, tok_ref, gain_ref, route_ref, target_ref, *rest):
    out_refs, normed_ref = rest[:-1], rest[-1]
    tok_rows, width = tok_ref.shape
    part = normed_ref.shape[1]
    experts = out_refs[0].shape[0]
    per = out_refs[0].shape[1]
    at = pl.ds(pl.multiple_of(me_ref[0] * part, part), part)
    block = 128
    for i in range(tok_rows // block):
        rows = slice(i * block, (i + 1) * block)
        widened = tok_ref[rows, :].astype(f32)
        scale = lax.rsqrt(jnp.mean(widened * widened, axis=-1, keepdims=True) + epsilon)
        mine = tok_ref[rows, at].astype(f32)
        normed_ref[rows, :] = ((mine * scale) * gain_ref[:, at]).astype(bf16)

    lanes = iota((tok_rows, 128), 1)
    first, second = route_ref[:, 0:1], route_ref[:, 1:2]
    named = (lanes == first) | (lanes == second)
    below = iota((tok_rows, tok_rows), 1) < iota((tok_rows, tok_rows), 0)
    earlier = dot(below.astype(bf16), named.astype(bf16))
    for c, chosen in enumerate((first, second)):
        slot = jnp.sum(jnp.where(lanes == chosen, earlier, 0.0), axis=1, keepdims=True).astype(jnp.int32)
        target_ref[:, c : c + 1] = (slot // per) * (experts * per) + chosen * per + slot % per
    code = jnp.where(named, earlier, -1.0).astype(bf16)
    rows_out = experts * per
    owner = (iota((rows_out, 128), 0) // per == iota((rows_out, 128), 1)).astype(bf16)
    spread = dot_t(owner, code)
    within = iota((rows_out, tok_rows), 0) % per
    for k, out_ref in enumerate(out_refs):
        pick = (spread == (within + k * per).astype(f32)).astype(bf16)
        out_ref[...] = dot(pick, normed_ref[...]).astype(bf16).reshape(out_ref.shape)


def order(me, n):
    return [me, lax.rem(me + n - 1, n), lax.rem(me + 1, n), lax.rem(me + 2, n)]


def hidden_kernel(me_ref, a_ref, b_ref, c_ref, d_ref, wg_ref, wu_ref, out_ref):
    part = a_ref.shape[1]
    gate, up = 0.0, 0.0
    for ref, owner in zip((a_ref, b_ref, c_ref, d_ref), order(me_ref[0], 4)):
        at = pl.ds(pl.multiple_of(owner * part, part), part)
        gate = gate + dot(ref[...], wg_ref[at, :])
        up = up + dot(ref[...], wu_ref[at, :])
    out_ref[...] = (gate * (1.0 / (1.0 + jnp.exp(-gate))) * up).astype(bf16)


def split_kernel(me_ref, wd_ref, *out_refs):
    part = out_refs[0].shape[1]
    for k, out_ref in enumerate(out_refs):
        owner = lax.rem(me_ref[0] + k, len(out_refs))
        out_ref[...] = wd_ref[:, pl.ds(pl.multiple_of(owner * part, part), part)]


def down_kernel(*refs):
    out_ref = refs[-1]
    n = (len(refs) - 1) // 2
    total = 0.0
    for ref, wd_ref in zip(refs[:n], refs[n : 2 * n]):
        total = total + dot(ref[...], wd_ref[...]).astype(bf16).astype(f32)
    out_ref[...] = total.astype(bf16)


def combine_kernel(target_ref, weight_ref, *rest):
    ret_refs, out_ref = rest[:-1], rest[-1]
    rows = ret_refs[0].shape[0]
    tok_rows = out_ref.shape[0]
    total = 0.0
    lanes = iota((tok_rows, rows), 1)
    for c in range(TOPK):
        target = target_ref[:, c : c + 1]
        picked = 0.0
        for k, ref in enumerate(ret_refs):
            pick = (lanes == target - k * rows).astype(bf16)
            picked = picked + dot(pick, ref[...])
        total = total + picked * weight_ref[:, c : c + 1]
    out_ref[...] = total.astype(bf16)


def smem():
    return pl.BlockSpec(memory_space=pltpu.SMEM)


def vmem():
    return pl.BlockSpec(memory_space=pltpu.VMEM)


def call(kernel, out_shape, args, flops, scratch=(), mib=48):
    outs = out_shape if isinstance(out_shape, (tuple, list)) else (out_shape,)
    moved = sum(a.size * a.dtype.itemsize for a in args) + sum(
        math.prod(o.shape) * o.dtype.itemsize for o in outs
    )
    return pl.pallas_call(
        kernel,
        out_shape=out_shape,
        in_specs=[smem() if a.size == 1 else vmem() for a in args],
        out_specs=jax.tree.map(lambda _: vmem(), out_shape),
        scratch_shapes=list(scratch),
        compiler_params=params(mib),
        cost_estimate=pl.CostEstimate(flops=flops, transcendentals=0, bytes_accessed=moved),
        name=kernel.__name__ if hasattr(kernel, "__name__") else "kernel",
    )(*args)


def shape(*dims, dtype=bf16):
    return jax.ShapeDtypeStruct(dims, dtype)


def body(
    query_latent,
    key_latent,
    rope_key,
    query_gain,
    key_gain,
    w_query,
    w_query_rope,
    w_key,
    w_value,
    w_out,
    tokens_b,
    ffn_gain,
    route_expert,
    route_weight,
    w_gate,
    w_up,
    w_down,
):
    tp = lax.axis_size("tp")
    experts = lax.axis_size("ep")
    me = lax.axis_index("tp").astype(jnp.int32).reshape(1)

    def ahead(k):
        return [(i, (i + k) % tp) for i in range(tp)]

    forward, backward = ahead(1), ahead(tp - 1)

    tok_a = query_latent.shape[0]
    heads = w_query.shape[1] // NOPE
    cosine, sine = rotary_lanes(tok_a)
    rank = key_latent.shape[1]
    send = call(
        latent_kernel,
        shape(tok_a, rank + 2 * ROPE),
        (key_latent, rope_key, key_gain.reshape(1, -1), cosine, sine),
        10**7,
    )
    latents = lax.all_gather(send, "ep", axis=0, tiled=True)

    tok_b, width = tokens_b.shape
    part = width // tp
    capacity = TOPK * tok_b // experts
    per = capacity // CHUNKS
    target, *outgoing = call(
        prep_kernel,
        [shape(tok_b, TOPK, dtype=jnp.int32)] + [shape(experts, per, part)] * CHUNKS,
        (me, tokens_b, ffn_gain.reshape(1, -1), route_expert),
        6 * 10**8,
        [pltpu.VMEM((tok_b, part), bf16)],
    )
    units = w_gate.shape[2]
    own, *sent = call(split_kernel, [shape(units, part)] * tp, (me, w_down[0]), 10**6)
    got = [lax.ppermute(piece, "tp", ahead(k + 1)) for k, piece in enumerate(sent)]
    *got, outgoing[1] = lax.optimization_barrier((*got, outgoing[1]))
    down = (own, got[0], got[2], got[1])

    queries = call(
        query_kernel,
        shape(heads, tok_a, NOPE + 2 * ROPE),
        (query_latent, query_gain.reshape(1, -1), w_query, w_query_rope, cosine, sine),
        10**8,
    )

    def spread(piece, k):
        before = lax.ppermute(piece, "tp", forward)
        after = lax.ppermute(piece, "tp", backward)
        if k % 2 == 0:
            opposite = lax.ppermute(before, "tp", forward)
        else:
            opposite = lax.ppermute(after, "tp", backward)
        return piece, before, after, opposite

    rows = experts * per
    arrived = [lax.all_to_all(o, "ep", 0, 0, tiled=True).reshape(rows, part) for o in outgoing]
    returned = []
    for k in range(CHUNKS):
        pieces = spread(arrived[k], k)
        hidden = call(
            hidden_kernel,
            shape(rows, units),
            (me, *pieces, w_gate[0], w_up[0]),
            4 * rows * width * units,
        )
        groups = spread(hidden, k)
        result = call(
            down_kernel,
            shape(rows, part),
            (*groups, *down),
            2 * rows * tp * units * part,
        )
        back = lax.all_to_all(result.reshape(experts, per, part), "ep", 0, 0, tiled=True)
        returned.append(back.reshape(rows, part))

    block = math.gcd(latents.shape[0], 1024)
    cols = latents.shape[1]
    share = shape(tok_a // tp, w_out.shape[1])
    shares = pl.pallas_call(
        attend_kernel,
        grid=(latents.shape[0] // block,),
        in_specs=[
            smem(),
            whole(queries.shape),
            pl.BlockSpec((block, cols), lambda i: (i, 0)),
            whole(w_key.shape),
            whole(w_value.shape),
            whole(w_out.shape),
        ],
        out_specs=[whole(share.shape)] * tp,
        out_shape=[share] * tp,
        scratch_shapes=[
            pltpu.VMEM((tok_a, w_out.shape[1]), bf16),
            pltpu.VMEM((heads, tok_a), f32),
            pltpu.VMEM((heads, tok_a), f32),
            pltpu.VMEM((heads, VDIM, tok_a), f32),
        ],
        compiler_params=params(48),
        cost_estimate=pl.CostEstimate(flops=6 * 10**9, transcendentals=2 * 10**6, bytes_accessed=8 * 10**6),
        name="attend",
    )(me, queries, latents, w_key, w_value, w_out)
    mine = [shares[0]] + [lax.ppermute(s, "tp", ahead(k)) for k, s in enumerate(shares) if k]
    mixer_out = sum(s.astype(f32) for s in mine).astype(bf16)

    moe_out = call(
        combine_kernel,
        shape(tok_b, part),
        (target, route_weight, *returned),
        4 * tok_b * rows * CHUNKS * part,
    )
    return (mixer_out, moe_out)


def solution(mesh):
    in_specs = (
        P("ep", None),
        P("ep", None),
        P("ep", None),
        P(),
        P(),
        P(None, "tp"),
        P(None, "tp"),
        P(None, "tp"),
        P(None, "tp"),
        P("tp", None),
        P("ep", None),
        P(),
        P("ep", None),
        P("ep", None),
        P("ep", None, "tp"),
        P("ep", None, "tp"),
        P("ep", "tp", None),
    )
    out_specs = (P(("ep", "tp"), None), P("ep", "tp"))
    return jax.shard_map(body, mesh=mesh, in_specs=in_specs, out_specs=out_specs, check_vma=False)
```

```python
import functools
import math

import jax
import jax.numpy as jnp
import numpy as np
from jax import lax
from jax.experimental import pallas as pl
from jax.experimental.pallas import tpu as pltpu
from jax.sharding import Mesh
from jax.sharding import PartitionSpec as P

NOPE = 128
ROPE = 64
VDIM = 128
GRID_W = 64
TOPK = 2
EP = ("z", "x", "c")
TP = ("yh", "yl")

epsilon = 1e-06
rotary_base = 10000.0
neg_large = -1e30
f32 = jnp.float32
bf16 = jnp.bfloat16


def params(mib):
    return pltpu.CompilerParams(vmem_limit_bytes=mib * 1024 * 1024)


def dot_t(a, b):
    return lax.dot_general(a, b, (((1,), (1,)), ((), ())), preferred_element_type=f32)


def dot_0(a, b):
    return lax.dot_general(a, b, (((0,), (0,)), ((), ())), preferred_element_type=f32)


def dot(a, b):
    return jnp.dot(a, b, preferred_element_type=f32)


def iota(shape, dim):
    return lax.broadcasted_iota(jnp.int32, shape, dim)


def rms(widened, gain):
    normed = widened * lax.rsqrt(jnp.mean(widened * widened, axis=-1, keepdims=True) + epsilon)
    return (normed * gain).astype(bf16)


def swap_matrix(n):
    row, col = iota((n, n), 0), iota((n, n), 1)
    minus = (row == col + 1) & (col % 2 == 0)
    plus = (row + 1 == col) & (col % 2 == 1)
    return (jnp.where(plus, 1.0, 0.0) - jnp.where(minus, 1.0, 0.0)).astype(bf16)


def latent_kernel(kl_ref, rk_ref, kg_ref, cos_ref, sin_ref, send_ref):
    normed = rms(kl_ref[...].astype(f32), kg_ref[...])
    turned = rk_ref[...].astype(f32) * cos_ref[...] + dot(rk_ref[...], swap_matrix(ROPE)) * sin_ref[...]
    ways = normed.shape[1] // ROPE
    few = normed.shape[0] // ways
    turned = turned.astype(bf16)
    lined = jnp.concatenate([turned[q * few : (q + 1) * few, :] for q in range(ways)], axis=1)
    send_ref[: normed.shape[0]] = normed
    send_ref[normed.shape[0] :] = lined


def join_kernel(*refs):
    out_ref = refs[-1]
    for i, ref in enumerate(refs[:-1]):
        out_ref[i] = ref[...]


def query_kernel(ql_ref, qg_ref, wq_ref, wqr_ref, cos_ref, sin_ref, q_ref):
    heads = q_ref.shape[0]
    normed = rms(ql_ref[...].astype(f32), qg_ref[...])
    nope = dot(normed, wq_ref[...]).astype(bf16)
    swapped = dot(wqr_ref[...], swap_matrix(heads * ROPE)).astype(bf16)
    plain = dot(normed, wqr_ref[...])
    other = dot(normed, swapped)
    for h in range(heads):
        at = slice(h * ROPE, (h + 1) * ROPE)
        rot = (plain[:, at] * cos_ref[...] + other[:, at] * sin_ref[...]).astype(bf16)
        q_ref[h] = jnp.concatenate([nope[:, h * NOPE : (h + 1) * NOPE], rot, jnp.zeros(rot.shape, bf16)], axis=1)


def attend_kernel(count, me_ref, q_ref, wk_ref, wv_ref, wo_ref, *refs):
    kv_refs, refs = refs[:count], refs[count:]
    out_refs, (kv_ref, all_ref, m_ref, l_ref, acc_ref, sem) = refs[:-6], refs[-6:]
    heads, tok_rows = q_ref.shape[:2]
    rank = wk_ref.shape[0]
    scale = (NOPE + ROPE) ** (-0.5)
    loads = [pltpu.make_async_copy(ref, kv_ref.at[i], sem.at[i]) for i, ref in enumerate(kv_refs)]
    for load in loads:
        load.start()
    m_ref[...] = jnp.full(m_ref.shape, neg_large, f32)
    l_ref[...] = jnp.zeros(l_ref.shape, f32)
    acc_ref[...] = jnp.zeros(acc_ref.shape, f32)
    blocks = kv_ref.shape[1]
    ways = rank // ROPE
    few = tok_rows // ways

    def step(j, carry):
        latent, turned = [], []
        for i in (2 * j, 2 * j + 1):
            pltpu.make_async_copy(kv_ref.at[i], kv_ref.at[i], sem.at[i]).wait()
            for q in range(ways):
                latent.append(kv_ref[i, :, q * few : (q + 1) * few, :].reshape(blocks * few, rank))
                part = kv_ref[i, :, tok_rows:, q * ROPE : (q + 1) * ROPE].reshape(blocks * few, ROPE)
                turned.append(jnp.concatenate([part, jnp.zeros(part.shape, bf16)], axis=1))
        latent = jnp.concatenate(latent, axis=0)
        turned = jnp.concatenate(turned, axis=0)
        keys = dot(latent, wk_ref[...]).astype(bf16)
        values = dot(latent, wv_ref[...]).astype(bf16)
        for h in range(heads):
            both = jnp.concatenate([keys[:, h * NOPE : (h + 1) * NOPE], turned], axis=1)
            scores = dot_t(both, q_ref[h]) * scale
            old = m_ref[h : h + 1, :]
            new = jnp.maximum(old, jnp.max(scores, axis=0, keepdims=True))
            weights = jnp.exp(scores - new)
            shrink = jnp.exp(old - new)
            m_ref[h : h + 1, :] = new
            l_ref[h : h + 1, :] = l_ref[h : h + 1, :] * shrink + jnp.sum(weights, axis=0, keepdims=True)
            added = dot_0(values[:, h * VDIM : (h + 1) * VDIM], weights.astype(bf16))
            acc_ref[h] = acc_ref[h] * shrink + added
        return carry

    lax.fori_loop(0, count // 2, step, 0)
    parts = [(acc_ref[h] / l_ref[h : h + 1, :]).astype(bf16) for h in range(heads)]
    all_ref[...] = dot_0(jnp.concatenate(parts, axis=0), wo_ref[...]).astype(bf16)
    share = tok_rows // len(out_refs)
    for k, out_ref in enumerate(out_refs):
        owner = lax.rem(me_ref[0] + k, len(out_refs))
        out_ref[...] = all_ref[pl.ds(pl.multiple_of(owner * share, share), share), :]


def rotary_lanes(tok_rows):
    positions = lax.axis_index(EP) * tok_rows + jnp.arange(tok_rows, dtype=jnp.int32)
    half = ROPE // 2
    inverse = rotary_base ** (-np.arange(0, half, 2, dtype=np.float32) / half)
    pair = np.arange(ROPE) // 2
    spread = jnp.asarray(inverse.astype(np.float32)[pair % (half // 2)])
    by_row = jnp.asarray(pair < half // 2)
    grid_row = (positions // GRID_W).astype(f32)
    grid_col = (positions % GRID_W).astype(f32)
    angle = jnp.where(by_row[None, :], grid_row[:, None], grid_col[:, None]) * spread[None, :]
    return jnp.cos(angle), jnp.sin(angle)


def prep_kernel(me_ref, tok_hbm, gain_hbm, route_hbm, target_ref, out_hbm, *scratch):
    tok_ref, gain_ref, route_ref, normed_ref, out_ref, load_sem, store_sem = scratch
    tok_rows, _ = tok_ref.shape
    part = normed_ref.shape[1]
    experts, per = out_ref.shape[:2]
    upper = me_ref[0] // 2
    half = (me_ref[0] // 2 + me_ref[0]) % 2
    at = pl.ds(pl.multiple_of(upper * part, part), part)
    blocks = 4
    block = tok_rows // blocks
    loads = [
        pltpu.make_async_copy(route_hbm, route_ref, load_sem.at[0]),
        pltpu.make_async_copy(gain_hbm, gain_ref, load_sem.at[1]),
    ]
    for i in range(blocks):
        rows = pl.ds(i * block, block)
        loads.append(pltpu.make_async_copy(tok_hbm.at[rows], tok_ref.at[rows], load_sem.at[2 + i]))
    for load in loads:
        load.start()

    loads[0].wait()
    names = iota((128, tok_rows), 0)
    first, second = route_ref[0:1, :], route_ref[1:2, :]
    named = (names == first) | (names == second)
    before = iota((tok_rows, tok_rows), 0) < iota((tok_rows, tok_rows), 1)
    earlier = dot(named.astype(bf16), before.astype(bf16))
    for c, chosen in enumerate((first, second)):
        slot = jnp.sum(jnp.where(names == chosen, earlier, 0.0), axis=0, keepdims=True).astype(jnp.int32)
        sender = (slot // per + upper) % 2
        target_ref[c : c + 1, :] = (chosen * 2 + sender) * per + slot % per
    code = jnp.where(named, earlier, -1.0).astype(bf16)

    loads[1].wait()
    for i in range(blocks):
        loads[2 + i].wait()
        rows = slice(i * block, (i + 1) * block)
        widened = tok_ref[rows, :].astype(f32)
        scale = lax.rsqrt(jnp.mean(widened * widened, axis=-1, keepdims=True) + epsilon)
        mine = tok_ref[rows, at].astype(f32)
        normed_ref[rows, :] = ((mine * scale) * gain_ref[:, at]).astype(bf16)

    share = experts // 2
    rows_out = share * per
    stores = []
    for i in range(2):
        owner = (iota((rows_out, 128), 0) // per + i * share == iota((rows_out, 128), 1)).astype(bf16)
        spread = dot(owner, code)
        within = iota((rows_out, tok_rows), 0) % per + half * per
        pick = (spread == within.astype(f32)).astype(bf16)
        out_ref[i * share : (i + 1) * share] = dot(pick, normed_ref[...]).astype(bf16).reshape(share, per, part)
        which = pl.ds(i * share, share)
        stores.append(pltpu.make_async_copy(out_ref.at[which], out_hbm.at[which], store_sem.at[i]))
        stores[-1].start()
    for store in stores:
        store.wait()


def half_kernel(me_ref, a_ref, wg_ref, wu_ref, vg_ref, vu_ref, *out_refs):
    part = a_ref.shape[1]
    units = wg_ref.shape[1]
    rows = out_refs[0].shape[0]
    at = pl.ds(pl.multiple_of(me_ref[0] // 2 * part, part), part)
    for i, out_ref in enumerate(out_refs):
        for k, ref in enumerate((wg_ref, wu_ref, vg_ref, vu_ref)):
            out_ref[:, k * units : (k + 1) * units] = dot(a_ref[i * rows : (i + 1) * rows, :], ref[at, :])


def hidden_kernel(me_ref, b_ref, wg_ref, wu_ref, vg_ref, vu_ref, held_ref, out_ref):
    part = b_ref.shape[1]
    units = wg_ref.shape[1]
    at = pl.ds(pl.multiple_of((1 - me_ref[0] // 2) * part, part), part)
    for k, (g_ref, u_ref) in enumerate(((wg_ref, wu_ref), (vg_ref, vu_ref))):
        cols = 2 * k * units
        gate = held_ref[:, cols : cols + units] + dot(b_ref[...], g_ref[at, :])
        up = held_ref[:, cols + units : cols + 2 * units] + dot(b_ref[...], u_ref[at, :])
        out_ref[:, k * units : (k + 1) * units] = (gate * (1.0 / (1.0 + jnp.exp(-gate))) * up).astype(bf16)


def split_kernel(me_ref, wd_ref, mine_ref, other_ref):
    part = mine_ref.shape[1]
    upper = me_ref[0] // 2
    mine_ref[...] = wd_ref[:, pl.ds(pl.multiple_of(upper * part, part), part)]
    other_ref[...] = wd_ref[:, pl.ds(pl.multiple_of((1 - upper) * part, part), part)]


def down_kernel(a_ref, b_ref, w0_ref, w1_ref, w2_ref, w3_ref, *rest):
    out_ref = rest[-1]
    units = w0_ref.shape[0]
    experts, ways, per, part = out_ref.shape
    fresh = a_ref.shape[0] // per
    if len(rest) > 1:
        out_ref[: experts - fresh] = rest[0][...]
    for y in range(ways):
        cols = slice(y * part, (y + 1) * part)
        total = 0.0
        for ref, k, wd_ref in ((a_ref, 0, w0_ref), (a_ref, 1, w1_ref), (b_ref, 0, w2_ref), (b_ref, 1, w3_ref)):
            term = dot(ref[:, k * units : (k + 1) * units], wd_ref[:, cols])
            total = total + term.astype(bf16).astype(f32)
        out_ref[experts - fresh :, y] = total.astype(bf16).reshape(fresh, per, part)


def combine_kernel(target_ref, weight_ref, *rest):
    ret_refs, out_ref = rest[:-1], rest[-1]
    rows = ret_refs[0].shape[0]
    tok_rows = out_ref.shape[0]
    total = 0.0
    lanes = iota((tok_rows, rows), 1)
    for c in range(TOPK):
        target = target_ref[:, c : c + 1]
        picked = 0.0
        for k, ref in enumerate(ret_refs):
            pick = (lanes == target - k * rows).astype(bf16)
            picked = picked + dot(pick, ref[...])
        total = total + picked * weight_ref[:, c : c + 1]
    out_ref[...] = total.astype(bf16)


def smem():
    return pl.BlockSpec(memory_space=pltpu.SMEM)


def vmem():
    return pl.BlockSpec(memory_space=pltpu.VMEM)


def call(kernel, out_shape, args, flops, scratch=(), mib=48):
    outs = out_shape if isinstance(out_shape, (tuple, list)) else (out_shape,)
    moved = sum(a.size * a.dtype.itemsize for a in args) + sum(
        math.prod(o.shape) * o.dtype.itemsize for o in outs
    )
    return pl.pallas_call(
        kernel,
        out_shape=out_shape,
        in_specs=[smem() if a.size == 1 else vmem() for a in args],
        out_specs=jax.tree.map(lambda _: vmem(), out_shape),
        scratch_shapes=list(scratch),
        compiler_params=params(mib),
        cost_estimate=pl.CostEstimate(flops=flops, transcendentals=0, bytes_accessed=moved),
    )(*args)


def shape(*dims, dtype=bf16):
    return jax.ShapeDtypeStruct(dims, dtype)


def inner(
    query_latent,
    key_latent,
    rope_key,
    query_gain,
    key_gain,
    w_query,
    w_query_rope,
    w_key,
    w_value,
    w_out,
    tokens_b,
    ffn_gain,
    route_expert,
    route_weight,
    w_gate,
    w_up,
    w_down,
):
    tp = lax.axis_size(TP)
    experts = lax.axis_size(EP)
    me = lax.axis_index(TP).astype(jnp.int32).reshape(1)

    def ahead(k, n=tp):
        return [(i, (i + k) % n) for i in range(n)]

    def across(k):
        return [(i, i ^ k) for i in range(tp)]

    far_gate = lax.ppermute(w_gate[0], TP, across(1))
    far_up = lax.ppermute(w_up[0], TP, across(1))

    tok_b, width = tokens_b.shape
    per = TOPK * tok_b // experts // 2
    part = width // 2
    rows = experts * per
    units = w_gate.shape[2]
    far = pl.BlockSpec(memory_space=pltpu.HBM)
    target, outgoing = pl.pallas_call(
        prep_kernel,
        out_shape=[shape(TOPK, tok_b, dtype=jnp.int32), shape(experts, per, part)],
        in_specs=[smem(), far, far, far],
        out_specs=[vmem(), far],
        scratch_shapes=[
            pltpu.VMEM((tok_b, width), bf16),
            pltpu.VMEM((1, width), f32),
            pltpu.VMEM((TOPK, tok_b), jnp.int32),
            pltpu.VMEM((tok_b, part), bf16),
            pltpu.VMEM((experts, per, part), bf16),
            pltpu.SemaphoreType.DMA((6,)),
            pltpu.SemaphoreType.DMA((2,)),
        ],
        compiler_params=params(48),
        cost_estimate=pl.CostEstimate(flops=6 * 10**8, transcendentals=0, bytes_accessed=4 * 10**6),
        name="prep",
    )(me, tokens_b, ffn_gain.reshape(1, -1), route_expert.T)
    arrived = lax.all_to_all(outgoing, EP, 0, 0, tiled=True)
    arrived = arrived.reshape(rows, part)

    mine, other = call(split_kernel, [shape(units, part)] * 2, (me, w_down[0]), 10**6)
    down3 = lax.ppermute(other, TP, across(3))
    down1 = lax.ppermute(mine, TP, across(1))
    down2 = lax.ppermute(down3, TP, across(1))
    down = (mine, down1, down3, down2)

    tok_a = query_latent.shape[0]
    heads = w_query.shape[1] // NOPE
    cosine, sine = rotary_lanes(tok_a)
    rank = key_latent.shape[1]
    sent = tok_a + tok_a * ROPE // rank
    depth = lax.axis_size("z")
    send = call(latent_kernel, shape(sent, rank), (key_latent, rope_key, key_gain.reshape(1, -1), cosine, sine), 10**7)
    wide = lax.axis_size("x")
    row = [send]
    for k in range(1, wide):
        row.append(lax.ppermute(send, "x", ahead(k, wide)))
    row = call(join_kernel, shape(wide, sent, rank), tuple(row), 10**6)
    queries = call(
        query_kernel,
        shape(heads, tok_a, NOPE + 2 * ROPE),
        (query_latent, query_gain.reshape(1, -1), w_query, w_query_rope, cosine, sine),
        10**8,
    )

    halves = 2
    few = rows // halves
    weights = (w_gate[0], w_up[0], far_gate, far_up)
    joined = []
    for i in range(halves):
        joined.append(lax.ppermute(arrived[i * few : (i + 1) * few], TP, across(3)))
    held = call(
        half_kernel, [shape(few, 4 * units, dtype=f32)] * halves, (me, arrived, *weights), 8 * rows * part * units
    )
    result = ()
    for i in range(halves):
        hidden = call(hidden_kernel, shape(few, 2 * units), (me, joined[i], *weights, held[i]), 8 * few * part * units)
        far_hidden = lax.ppermute(hidden, TP, across(3))
        result = (
            call(
                down_kernel,
                shape(experts * (i + 1) // halves, 2, per, part // 2),
                (hidden, far_hidden, *down, *result),
                8 * few * units * part,
            ),
        )
    result = result[0]

    near = [row]
    up, low = row, row
    for k in range(1, depth // 2 + 1):
        up = lax.ppermute(up, "z", ahead(1, depth))
        near.append(up)
        if 2 * k < depth:
            low = lax.ppermute(low, "z", ahead(depth - 1, depth))
            near.append(low)
    pieces = []
    for piece in near[:depth]:
        pieces += [piece, lax.ppermute(piece, "c", [(0, 1), (1, 0)])]

    share = shape(tok_a // tp, w_out.shape[1])
    count = len(pieces)
    shares = pl.pallas_call(
        functools.partial(attend_kernel, count),
        out_shape=[share] * tp,
        in_specs=[smem()] + [vmem()] * 4 + [far] * count,
        out_specs=[vmem()] * tp,
        scratch_shapes=[
            pltpu.VMEM((count, *pieces[0].shape), bf16),
            pltpu.VMEM((tok_a, w_out.shape[1]), bf16),
            pltpu.VMEM((heads, tok_a), f32),
            pltpu.VMEM((heads, tok_a), f32),
            pltpu.VMEM((heads, VDIM, tok_a), f32),
            pltpu.SemaphoreType.DMA((count,)),
        ],
        compiler_params=params(48),
        cost_estimate=pl.CostEstimate(flops=6 * 10**9, transcendentals=0, bytes_accessed=8 * 10**6),
        name="attend",
    )(me, queries, w_key, w_value, w_out, *pieces)
    held = [shares[0]] + [lax.ppermute(s, TP, ahead(k)) for k, s in enumerate(shares) if k]
    mixer_out = sum(s.astype(f32) for s in held).astype(bf16)

    returned = lax.all_to_all(result.reshape(2 * experts, per, part // 2), (*EP, "yl"), 0, 0, tiled=True)
    moe_out = call(
        combine_kernel,
        shape(tok_b, part // 2),
        (target.T, route_weight, returned.reshape(2 * rows, part // 2)),
        4 * tok_b * 2 * rows * part // 2,
    )
    return (mixer_out, moe_out)


def spec(*dims):
    spread = {"ep": EP, "tp": TP, "both": EP + TP}
    return P(*(spread.get(d) for d in dims))


def solution(mesh):
    ep, tp = mesh.devices.shape
    fine = Mesh(mesh.devices.reshape(ep // 8, 4, 2, tp // 2, 2), EP + TP)
    in_specs = (
        spec("ep", None),
        spec("ep", None),
        spec("ep", None),
        spec(),
        spec(),
        spec(None, "tp"),
        spec(None, "tp"),
        spec(None, "tp"),
        spec(None, "tp"),
        spec("tp", None),
        spec("ep", None),
        spec(),
        spec("ep", None),
        spec("ep", None),
        spec("ep", None, "tp"),
        spec("ep", None, "tp"),
        spec("ep", "tp", None),
    )
    out_specs = (spec("both", None), spec("ep", "tp"))
    return jax.shard_map(inner, mesh=fine, in_specs=in_specs, out_specs=out_specs, check_vma=False)
```

```python
import functools
import math

import jax
import jax.numpy as jnp
import numpy as np
from jax import lax
from jax.experimental import pallas as pl
from jax.experimental.pallas import tpu as pltpu
from jax.sharding import Mesh
from jax.sharding import PartitionSpec as P

NOPE = 128
ROPE = 64
VDIM = 128
GRID_W = 64
TOPK = 2
EP = ("z", "x", "c")
TP = ("yh", "yl")

epsilon = 1e-06
rotary_base = 10000.0
neg_large = -1e30
f32 = jnp.float32
bf16 = jnp.bfloat16


def params(mib):
    return pltpu.CompilerParams(vmem_limit_bytes=mib * 1024 * 1024)


def dot_t(a, b):
    return lax.dot_general(a, b, (((1,), (1,)), ((), ())), preferred_element_type=f32)


def dot_0(a, b):
    return lax.dot_general(a, b, (((0,), (0,)), ((), ())), preferred_element_type=f32)


def dot(a, b):
    return jnp.dot(a, b, preferred_element_type=f32)


def iota(shape, dim):
    return lax.broadcasted_iota(jnp.int32, shape, dim)


def rms(widened, gain):
    normed = widened * lax.rsqrt(jnp.mean(widened * widened, axis=-1, keepdims=True) + epsilon)
    return (normed * gain).astype(bf16)


def swap_matrix(n):
    row, col = iota((n, n), 0), iota((n, n), 1)
    minus = (row == col + 1) & (col % 2 == 0)
    plus = (row + 1 == col) & (col % 2 == 1)
    return (jnp.where(plus, 1.0, 0.0) - jnp.where(minus, 1.0, 0.0)).astype(bf16)


def latent_kernel(kl_ref, rk_ref, kg_ref, cos_ref, sin_ref, send_ref):
    normed = rms(kl_ref[...].astype(f32), kg_ref[...])
    turned = rk_ref[...].astype(f32) * cos_ref[...] + dot(rk_ref[...], swap_matrix(ROPE)) * sin_ref[...]
    ways = normed.shape[1] // ROPE
    few = normed.shape[0] // ways
    turned = turned.astype(bf16)
    lined = jnp.concatenate([turned[q * few : (q + 1) * few, :] for q in range(ways)], axis=1)
    send_ref[: normed.shape[0]] = normed
    send_ref[normed.shape[0] :] = lined


def join_kernel(*refs):
    out_ref = refs[-1]
    for i, ref in enumerate(refs[:-1]):
        out_ref[i] = ref[...]


def query_kernel(ql_ref, qg_ref, wq_ref, wqr_ref, cos_ref, sin_ref, q_ref):
    heads = q_ref.shape[0]
    normed = rms(ql_ref[...].astype(f32), qg_ref[...])
    nope = dot(normed, wq_ref[...]).astype(bf16)
    swapped = dot(wqr_ref[...], swap_matrix(heads * ROPE)).astype(bf16)
    plain = dot(normed, wqr_ref[...])
    other = dot(normed, swapped)
    for h in range(heads):
        at = slice(h * ROPE, (h + 1) * ROPE)
        rot = (plain[:, at] * cos_ref[...] + other[:, at] * sin_ref[...]).astype(bf16)
        q_ref[h] = jnp.concatenate([nope[:, h * NOPE : (h + 1) * NOPE], rot, jnp.zeros(rot.shape, bf16)], axis=1)


def attend_kernel(count, me_ref, q_ref, wk_ref, wv_ref, wo_ref, *refs):
    kv_refs, refs = refs[:count], refs[count:]
    out_refs, (kv_ref, all_ref, m_ref, l_ref, acc_ref, sem) = refs[:-6], refs[-6:]
    heads, tok_rows = q_ref.shape[:2]
    rank = wk_ref.shape[0]
    scale = (NOPE + ROPE) ** (-0.5)
    loads = [pltpu.make_async_copy(ref, kv_ref.at[i], sem.at[i]) for i, ref in enumerate(kv_refs)]
    for load in loads:
        load.start()
    m_ref[...] = jnp.full(m_ref.shape, neg_large, f32)
    l_ref[...] = jnp.zeros(l_ref.shape, f32)
    acc_ref[...] = jnp.zeros(acc_ref.shape, f32)
    blocks = kv_ref.shape[1]
    ways = rank // ROPE
    few = tok_rows // ways
    group = 4

    def step(j, carry):
        latent, turned = [], []
        for i in (group * j + k for k in range(group)):
            pltpu.make_async_copy(kv_ref.at[i], kv_ref.at[i], sem.at[i]).wait()
            for q in range(ways):
                latent.append(kv_ref[i, :, q * few : (q + 1) * few, :].reshape(blocks * few, rank))
                part = kv_ref[i, :, tok_rows:, q * ROPE : (q + 1) * ROPE].reshape(blocks * few, ROPE)
                turned.append(jnp.concatenate([part, jnp.zeros(part.shape, bf16)], axis=1))
        latent = jnp.concatenate(latent, axis=0)
        turned = jnp.concatenate(turned, axis=0)
        keys = dot(latent, wk_ref[...]).astype(bf16)
        values = dot(latent, wv_ref[...]).astype(bf16)
        for h in range(heads):
            both = jnp.concatenate([keys[:, h * NOPE : (h + 1) * NOPE], turned], axis=1)
            scores = dot_t(both, q_ref[h]) * scale
            old = m_ref[h : h + 1, :]
            new = jnp.maximum(old, jnp.max(scores, axis=0, keepdims=True))
            weights = jnp.exp(scores - new)
            shrink = jnp.exp(old - new)
            m_ref[h : h + 1, :] = new
            l_ref[h : h + 1, :] = l_ref[h : h + 1, :] * shrink + jnp.sum(weights, axis=0, keepdims=True)
            added = dot_0(values[:, h * VDIM : (h + 1) * VDIM], weights.astype(bf16))
            acc_ref[h] = acc_ref[h] * shrink + added
        return carry

    lax.fori_loop(0, count // group, step, 0)
    parts = [(acc_ref[h] / l_ref[h : h + 1, :]).astype(bf16) for h in range(heads)]
    all_ref[...] = dot_0(jnp.concatenate(parts, axis=0), wo_ref[...]).astype(bf16)
    share = tok_rows // len(out_refs)
    for k, out_ref in enumerate(out_refs):
        owner = lax.rem(me_ref[0] + k, len(out_refs))
        out_ref[...] = all_ref[pl.ds(pl.multiple_of(owner * share, share), share), :]


def rotary_lanes(tok_rows):
    positions = lax.axis_index(EP) * tok_rows + jnp.arange(tok_rows, dtype=jnp.int32)
    half = ROPE // 2
    inverse = rotary_base ** (-np.arange(0, half, 2, dtype=np.float32) / half)
    pair = np.arange(ROPE) // 2
    spread = jnp.asarray(inverse.astype(np.float32)[pair % (half // 2)])
    by_row = jnp.asarray(pair < half // 2)
    grid_row = (positions // GRID_W).astype(f32)
    grid_col = (positions % GRID_W).astype(f32)
    angle = jnp.where(by_row[None, :], grid_row[:, None], grid_col[:, None]) * spread[None, :]
    return jnp.cos(angle), jnp.sin(angle)


def prep_kernel(me_ref, tok_hbm, gain_hbm, route_hbm, target_ref, out_hbm, *scratch):
    tok_ref, gain_ref, route_ref, normed_ref, out_ref, load_sem, store_sem = scratch
    tok_rows, _ = tok_ref.shape
    part = normed_ref.shape[1]
    experts, per = out_ref.shape[:2]
    upper = me_ref[0] // 2
    half = (me_ref[0] // 2 + me_ref[0]) % 2
    at = pl.ds(pl.multiple_of(upper * part, part), part)
    blocks = 4
    block = tok_rows // blocks
    loads = [
        pltpu.make_async_copy(route_hbm, route_ref, load_sem.at[0]),
        pltpu.make_async_copy(gain_hbm, gain_ref, load_sem.at[1]),
    ]
    for i in range(blocks):
        rows = pl.ds(i * block, block)
        loads.append(pltpu.make_async_copy(tok_hbm.at[rows], tok_ref.at[rows], load_sem.at[2 + i]))
    for load in loads:
        load.start()

    loads[0].wait()
    names = iota((128, tok_rows), 0)
    first, second = route_ref[0:1, :], route_ref[1:2, :]
    named = (names == first) | (names == second)
    before = iota((tok_rows, tok_rows), 0) < iota((tok_rows, tok_rows), 1)
    earlier = dot(named.astype(bf16), before.astype(bf16))
    for c, chosen in enumerate((first, second)):
        slot = jnp.sum(jnp.where(names == chosen, earlier, 0.0), axis=0, keepdims=True).astype(jnp.int32)
        sender = (slot // per + upper) % 2
        target_ref[c : c + 1, :] = (chosen * 2 + sender) * per + slot % per
    code = jnp.where(named, earlier, -1.0).astype(bf16)

    loads[1].wait()
    for i in range(blocks):
        loads[2 + i].wait()
        rows = slice(i * block, (i + 1) * block)
        widened = tok_ref[rows, :].astype(f32)
        scale = lax.rsqrt(jnp.mean(widened * widened, axis=-1, keepdims=True) + epsilon)
        mine = tok_ref[rows, at].astype(f32)
        normed_ref[rows, :] = ((mine * scale) * gain_ref[:, at]).astype(bf16)

    share = experts // 2
    rows_out = share * per
    stores = []
    for i in range(2):
        owner = (iota((rows_out, 128), 0) // per + i * share == iota((rows_out, 128), 1)).astype(bf16)
        spread = dot(owner, code)
        within = iota((rows_out, tok_rows), 0) % per + half * per
        pick = (spread == within.astype(f32)).astype(bf16)
        out_ref[i * share : (i + 1) * share] = dot(pick, normed_ref[...]).astype(bf16).reshape(share, per, part)
        which = pl.ds(i * share, share)
        stores.append(pltpu.make_async_copy(out_ref.at[which], out_hbm.at[which], store_sem.at[i]))
        stores[-1].start()
    for store in stores:
        store.wait()


def half_kernel(me_ref, a_ref, wg_ref, wu_ref, vg_ref, vu_ref, *out_refs):
    part = a_ref.shape[1]
    units = wg_ref.shape[1]
    rows = out_refs[0].shape[0]
    at = pl.ds(pl.multiple_of(me_ref[0] // 2 * part, part), part)
    for i, out_ref in enumerate(out_refs):
        for k, ref in enumerate((wg_ref, wu_ref, vg_ref, vu_ref)):
            out_ref[:, k * units : (k + 1) * units] = dot(a_ref[i * rows : (i + 1) * rows, :], ref[at, :])


def hidden_kernel(me_ref, b_ref, wg_ref, wu_ref, vg_ref, vu_ref, held_ref, out_ref):
    part = b_ref.shape[1]
    units = wg_ref.shape[1]
    at = pl.ds(pl.multiple_of((1 - me_ref[0] // 2) * part, part), part)
    for k, (g_ref, u_ref) in enumerate(((wg_ref, wu_ref), (vg_ref, vu_ref))):
        cols = 2 * k * units
        gate = held_ref[:, cols : cols + units] + dot(b_ref[...], g_ref[at, :])
        up = held_ref[:, cols + units : cols + 2 * units] + dot(b_ref[...], u_ref[at, :])
        out_ref[:, k * units : (k + 1) * units] = (gate * (1.0 / (1.0 + jnp.exp(-gate))) * up).astype(bf16)


def split_kernel(me_ref, wd_ref, mine_ref, other_ref):
    part = mine_ref.shape[1]
    upper = me_ref[0] // 2
    mine_ref[...] = wd_ref[:, pl.ds(pl.multiple_of(upper * part, part), part)]
    other_ref[...] = wd_ref[:, pl.ds(pl.multiple_of((1 - upper) * part, part), part)]


def down_kernel(a_ref, b_ref, w0_ref, w1_ref, w2_ref, w3_ref, *rest):
    out_ref = rest[-1]
    units = w0_ref.shape[0]
    experts, ways, per, part = out_ref.shape
    fresh = a_ref.shape[0] // per
    if len(rest) > 1:
        out_ref[: experts - fresh] = rest[0][...]
    for y in range(ways):
        cols = slice(y * part, (y + 1) * part)
        total = 0.0
        for ref, k, wd_ref in ((a_ref, 0, w0_ref), (a_ref, 1, w1_ref), (b_ref, 0, w2_ref), (b_ref, 1, w3_ref)):
            term = dot(ref[:, k * units : (k + 1) * units], wd_ref[:, cols])
            total = total + term.astype(bf16).astype(f32)
        out_ref[experts - fresh :, y] = total.astype(bf16).reshape(fresh, per, part)


def combine_kernel(target_ref, weight_ref, *rest):
    ret_refs, out_ref = rest[:-1], rest[-1]
    rows = ret_refs[0].shape[0]
    tok_rows = out_ref.shape[0]
    total = 0.0
    lanes = iota((tok_rows, rows), 1)
    for c in range(TOPK):
        target = target_ref[:, c : c + 1]
        picked = 0.0
        for k, ref in enumerate(ret_refs):
            pick = (lanes == target - k * rows).astype(bf16)
            picked = picked + dot(pick, ref[...])
        total = total + picked * weight_ref[:, c : c + 1]
    out_ref[...] = total.astype(bf16)


def smem():
    return pl.BlockSpec(memory_space=pltpu.SMEM)


def vmem():
    return pl.BlockSpec(memory_space=pltpu.VMEM)


def call(kernel, out_shape, args, flops, scratch=(), mib=48):
    outs = out_shape if isinstance(out_shape, (tuple, list)) else (out_shape,)
    moved = sum(a.size * a.dtype.itemsize for a in args) + sum(
        math.prod(o.shape) * o.dtype.itemsize for o in outs
    )
    return pl.pallas_call(
        kernel,
        out_shape=out_shape,
        in_specs=[smem() if a.size == 1 else vmem() for a in args],
        out_specs=jax.tree.map(lambda _: vmem(), out_shape),
        scratch_shapes=list(scratch),
        compiler_params=params(mib),
        cost_estimate=pl.CostEstimate(flops=flops, transcendentals=0, bytes_accessed=moved),
    )(*args)


def shape(*dims, dtype=bf16):
    return jax.ShapeDtypeStruct(dims, dtype)


def inner(
    query_latent,
    key_latent,
    rope_key,
    query_gain,
    key_gain,
    w_query,
    w_query_rope,
    w_key,
    w_value,
    w_out,
    tokens_b,
    ffn_gain,
    route_expert,
    route_weight,
    w_gate,
    w_up,
    w_down,
):
    tp = lax.axis_size(TP)
    experts = lax.axis_size(EP)
    me = lax.axis_index(TP).astype(jnp.int32).reshape(1)

    def ahead(k, n=tp):
        return [(i, (i + k) % n) for i in range(n)]

    def across(k):
        return [(i, i ^ k) for i in range(tp)]

    far_gate = lax.ppermute(w_gate[0], TP, across(1))
    far_up = lax.ppermute(w_up[0], TP, across(1))

    tok_b, width = tokens_b.shape
    per = TOPK * tok_b // experts // 2
    part = width // 2
    rows = experts * per
    units = w_gate.shape[2]
    far = pl.BlockSpec(memory_space=pltpu.HBM)
    target, outgoing = pl.pallas_call(
        prep_kernel,
        out_shape=[shape(TOPK, tok_b, dtype=jnp.int32), shape(experts, per, part)],
        in_specs=[smem(), far, far, far],
        out_specs=[vmem(), far],
        scratch_shapes=[
            pltpu.VMEM((tok_b, width), bf16),
            pltpu.VMEM((1, width), f32),
            pltpu.VMEM((TOPK, tok_b), jnp.int32),
            pltpu.VMEM((tok_b, part), bf16),
            pltpu.VMEM((experts, per, part), bf16),
            pltpu.SemaphoreType.DMA((6,)),
            pltpu.SemaphoreType.DMA((2,)),
        ],
        compiler_params=params(48),
        cost_estimate=pl.CostEstimate(flops=6 * 10**8, transcendentals=0, bytes_accessed=4 * 10**6),
        name="prep",
    )(
        me,
        pltpu.with_memory_space_constraint(tokens_b, pltpu.HBM),
        pltpu.with_memory_space_constraint(ffn_gain.reshape(1, -1), pltpu.HBM),
        pltpu.with_memory_space_constraint(route_expert.T, pltpu.HBM),
    )
    arrived = lax.all_to_all(outgoing, EP, 0, 0, tiled=True)
    arrived = arrived.reshape(rows, part)

    mine, other = call(split_kernel, [shape(units, part)] * 2, (me, w_down[0]), 10**6)
    down3 = lax.ppermute(other, TP, across(3))
    down1 = lax.ppermute(mine, TP, across(1))
    down2 = lax.ppermute(down3, TP, across(1))
    down = (mine, down1, down3, down2)

    tok_a = query_latent.shape[0]
    heads = w_query.shape[1] // NOPE
    cosine, sine = rotary_lanes(tok_a)
    rank = key_latent.shape[1]
    sent = tok_a + tok_a * ROPE // rank
    depth = lax.axis_size("z")
    send = call(latent_kernel, shape(sent, rank), (key_latent, rope_key, key_gain.reshape(1, -1), cosine, sine), 10**7)
    wide = lax.axis_size("x")
    row = [send]
    for k in range(1, wide):
        row.append(lax.ppermute(send, "x", ahead(k, wide)))
    row = call(join_kernel, shape(wide, sent, rank), tuple(row), 10**6)
    queries = call(
        query_kernel,
        shape(heads, tok_a, NOPE + 2 * ROPE),
        (query_latent, query_gain.reshape(1, -1), w_query, w_query_rope, cosine, sine),
        10**8,
    )

    halves = 2
    few = rows // halves
    weights = (w_gate[0], w_up[0], far_gate, far_up)
    joined = []
    for i in range(halves):
        joined.append(lax.ppermute(arrived[i * few : (i + 1) * few], TP, across(3)))
    held = call(
        half_kernel, [shape(few, 4 * units, dtype=f32)] * halves, (me, arrived, *weights), 8 * rows * part * units
    )
    result = ()
    for i in range(halves):
        hidden = call(hidden_kernel, shape(few, 2 * units), (me, joined[i], *weights, held[i]), 8 * few * part * units)
        far_hidden = lax.ppermute(hidden, TP, across(3))
        result = (
            call(
                down_kernel,
                shape(experts * (i + 1) // halves, 2, per, part // 2),
                (hidden, far_hidden, *down, *result),
                8 * few * units * part,
            ),
        )
    result = result[0]

    near = [row]
    up, low = row, row
    for k in range(1, depth // 2 + 1):
        up = lax.ppermute(up, "z", ahead(1, depth))
        near.append(up)
        if 2 * k < depth:
            low = lax.ppermute(low, "z", ahead(depth - 1, depth))
            near.append(low)
    pieces = []
    for piece in near:
        pieces += [piece, lax.ppermute(piece, "c", [(0, 1), (1, 0)])]

    share = shape(tok_a // tp, w_out.shape[1])
    count = len(pieces)
    shares = pl.pallas_call(
        functools.partial(attend_kernel, count),
        out_shape=[share] * tp,
        in_specs=[smem()] + [vmem()] * 4 + [far] * count,
        out_specs=[vmem()] * tp,
        scratch_shapes=[
            pltpu.VMEM((count, *pieces[0].shape), bf16),
            pltpu.VMEM((tok_a, w_out.shape[1]), bf16),
            pltpu.VMEM((heads, tok_a), f32),
            pltpu.VMEM((heads, tok_a), f32),
            pltpu.VMEM((heads, VDIM, tok_a), f32),
            pltpu.SemaphoreType.DMA((count,)),
        ],
        compiler_params=params(48),
        cost_estimate=pl.CostEstimate(flops=6 * 10**9, transcendentals=0, bytes_accessed=8 * 10**6),
        name="attend",
    )(me, queries, w_key, w_value, w_out, *pieces)
    held = [shares[0]] + [lax.ppermute(s, TP, ahead(k)) for k, s in enumerate(shares) if k]
    mixer_out = sum(s.astype(f32) for s in held).astype(bf16)

    returned = lax.all_to_all(result.reshape(2 * experts, per, part // 2), (*EP, "yl"), 0, 0, tiled=True)
    moe_out = call(
        combine_kernel,
        shape(tok_b, part // 2),
        (target.T, route_weight, returned.reshape(2 * rows, part // 2)),
        4 * tok_b * 2 * rows * part // 2,
    )
    return (mixer_out, moe_out)


def spec(*dims):
    spread = {"ep": EP, "tp": TP, "both": EP + TP}
    return P(*(spread.get(d) for d in dims))


def solution(mesh):
    ep, tp = mesh.devices.shape
    fine = Mesh(mesh.devices.reshape(ep // 8, 4, 2, tp // 2, 2), EP + TP)
    in_specs = (
        spec("ep", None),
        spec("ep", None),
        spec("ep", None),
        spec(),
        spec(),
        spec(None, "tp"),
        spec(None, "tp"),
        spec(None, "tp"),
        spec(None, "tp"),
        spec("tp", None),
        spec("ep", None),
        spec(),
        spec("ep", None),
        spec("ep", None),
        spec("ep", None, "tp"),
        spec("ep", None, "tp"),
        spec("ep", "tp", None),
    )
    out_specs = (spec("both", None), spec("ep", "tp"))
    return jax.shard_map(inner, mesh=fine, in_specs=in_specs, out_specs=out_specs, check_vma=False)
```

```python
import functools
import math

import jax
import jax.numpy as jnp
import numpy as np
from jax import lax
from jax.experimental import pallas as pl
from jax.experimental.pallas import tpu as pltpu
from jax.sharding import Mesh
from jax.sharding import PartitionSpec as P

NOPE = 128
ROPE = 64
VDIM = 128
GRID_W = 64
TOPK = 2
EP = ("z", "x", "c")
TP = ("yh", "yl")

epsilon = 1e-06
rotary_base = 10000.0
neg_large = -1e30
f32 = jnp.float32
bf16 = jnp.bfloat16


def params(mib):
    return pltpu.CompilerParams(vmem_limit_bytes=mib * 1024 * 1024)


def dot_t(a, b):
    return lax.dot_general(a, b, (((1,), (1,)), ((), ())), preferred_element_type=f32)


def dot_0(a, b):
    return lax.dot_general(a, b, (((0,), (0,)), ((), ())), preferred_element_type=f32)


def dot(a, b):
    return jnp.dot(a, b, preferred_element_type=f32)


def iota(shape, dim):
    return lax.broadcasted_iota(jnp.int32, shape, dim)


def rms(widened, gain):
    normed = widened * lax.rsqrt(jnp.mean(widened * widened, axis=-1, keepdims=True) + epsilon)
    return (normed * gain).astype(bf16)


def swap_matrix(n):
    row, col = iota((n, n), 0), iota((n, n), 1)
    minus = (row == col + 1) & (col % 2 == 0)
    plus = (row + 1 == col) & (col % 2 == 1)
    return (jnp.where(plus, 1.0, 0.0) - jnp.where(minus, 1.0, 0.0)).astype(bf16)


def latent_kernel(kl_ref, rk_ref, kg_ref, cos_ref, sin_ref, send_ref):
    normed = rms(kl_ref[...].astype(f32), kg_ref[...])
    turned = rk_ref[...].astype(f32) * cos_ref[...] + dot(rk_ref[...], swap_matrix(ROPE)) * sin_ref[...]
    ways = normed.shape[1] // ROPE
    few = normed.shape[0] // ways
    turned = turned.astype(bf16)
    lined = jnp.concatenate([turned[q * few : (q + 1) * few, :] for q in range(ways)], axis=1)
    send_ref[: normed.shape[0]] = normed
    send_ref[normed.shape[0] :] = lined


def join_kernel(*refs):
    out_ref = refs[-1]
    for i, ref in enumerate(refs[:-1]):
        out_ref[i] = ref[...]


def query_kernel(ql_ref, qg_ref, wq_ref, wqr_ref, cos_ref, sin_ref, q_ref):
    heads = q_ref.shape[0]
    normed = rms(ql_ref[...].astype(f32), qg_ref[...])
    nope = dot(normed, wq_ref[...]).astype(bf16)
    swapped = dot(wqr_ref[...], swap_matrix(heads * ROPE)).astype(bf16)
    plain = dot(normed, wqr_ref[...])
    other = dot(normed, swapped)
    for h in range(heads):
        at = slice(h * ROPE, (h + 1) * ROPE)
        rot = (plain[:, at] * cos_ref[...] + other[:, at] * sin_ref[...]).astype(bf16)
        q_ref[h] = jnp.concatenate([nope[:, h * NOPE : (h + 1) * NOPE], rot, jnp.zeros(rot.shape, bf16)], axis=1)


def attend_kernel(count, me_ref, q_ref, wk_ref, wv_ref, wo_ref, *refs):
    kv_refs, refs = refs[:count], refs[count:]
    out_refs, (kv_ref, all_ref, m_ref, l_ref, acc_ref, sem) = refs[:-6], refs[-6:]
    heads, tok_rows = q_ref.shape[:2]
    rank = wk_ref.shape[0]
    scale = (NOPE + ROPE) ** (-0.5)
    loads = [pltpu.make_async_copy(ref, kv_ref.at[i], sem.at[i]) for i, ref in enumerate(kv_refs)]
    for load in loads:
        load.start()
    m_ref[...] = jnp.full(m_ref.shape, neg_large, f32)
    l_ref[...] = jnp.zeros(l_ref.shape, f32)
    acc_ref[...] = jnp.zeros(acc_ref.shape, f32)
    blocks = kv_ref.shape[1]
    ways = rank // ROPE
    few = tok_rows // ways
    group = 8

    def step(j, carry):
        latent, turned = [], []
        for i in (group * j + k for k in range(group)):
            pltpu.make_async_copy(kv_ref.at[i], kv_ref.at[i], sem.at[i]).wait()
            for q in range(ways):
                latent.append(kv_ref[i, :, q * few : (q + 1) * few, :].reshape(blocks * few, rank))
                part = kv_ref[i, :, tok_rows:, q * ROPE : (q + 1) * ROPE].reshape(blocks * few, ROPE)
                turned.append(jnp.concatenate([part, jnp.zeros(part.shape, bf16)], axis=1))
        latent = jnp.concatenate(latent, axis=0)
        turned = jnp.concatenate(turned, axis=0)
        keys = dot(latent, wk_ref[...]).astype(bf16)
        values = dot(latent, wv_ref[...]).astype(bf16)
        for h in range(heads):
            both = jnp.concatenate([keys[:, h * NOPE : (h + 1) * NOPE], turned], axis=1)
            scores = dot_t(both, q_ref[h]) * scale
            old = m_ref[h : h + 1, :]
            new = jnp.maximum(old, jnp.max(scores, axis=0, keepdims=True))
            weights = jnp.exp(scores - new)
            shrink = jnp.exp(old - new)
            m_ref[h : h + 1, :] = new
            l_ref[h : h + 1, :] = l_ref[h : h + 1, :] * shrink + jnp.sum(weights, axis=0, keepdims=True)
            added = dot_0(values[:, h * VDIM : (h + 1) * VDIM], weights.astype(bf16))
            acc_ref[h] = acc_ref[h] * shrink + added
        return carry

    lax.fori_loop(0, count // group, step, 0)
    parts = [(acc_ref[h] / l_ref[h : h + 1, :]).astype(bf16) for h in range(heads)]
    all_ref[...] = dot_0(jnp.concatenate(parts, axis=0), wo_ref[...]).astype(bf16)
    share = tok_rows // len(out_refs)
    for k, out_ref in enumerate(out_refs):
        owner = lax.rem(me_ref[0] + k, len(out_refs))
        out_ref[...] = all_ref[pl.ds(pl.multiple_of(owner * share, share), share), :]


def rotary_lanes(tok_rows):
    positions = lax.axis_index(EP) * tok_rows + jnp.arange(tok_rows, dtype=jnp.int32)
    half = ROPE // 2
    inverse = rotary_base ** (-np.arange(0, half, 2, dtype=np.float32) / half)
    pair = np.arange(ROPE) // 2
    spread = jnp.asarray(inverse.astype(np.float32)[pair % (half // 2)])
    by_row = jnp.asarray(pair < half // 2)
    grid_row = (positions // GRID_W).astype(f32)
    grid_col = (positions % GRID_W).astype(f32)
    angle = jnp.where(by_row[None, :], grid_row[:, None], grid_col[:, None]) * spread[None, :]
    return jnp.cos(angle), jnp.sin(angle)


def prep_kernel(me_ref, tok_hbm, gain_hbm, route_hbm, target_ref, out_hbm, *scratch):
    tok_ref, gain_ref, route_ref, normed_ref, out_ref, load_sem, store_sem = scratch
    tok_rows, _ = tok_ref.shape
    part = normed_ref.shape[1]
    experts, per = out_ref.shape[:2]
    upper = me_ref[0] // 2
    half = (me_ref[0] // 2 + me_ref[0]) % 2
    at = pl.ds(pl.multiple_of(upper * part, part), part)
    blocks = 4
    block = tok_rows // blocks
    loads = [
        pltpu.make_async_copy(route_hbm, route_ref, load_sem.at[0]),
        pltpu.make_async_copy(gain_hbm, gain_ref, load_sem.at[1]),
    ]
    for i in range(blocks):
        rows = pl.ds(i * block, block)
        loads.append(pltpu.make_async_copy(tok_hbm.at[rows], tok_ref.at[rows], load_sem.at[2 + i]))
    for load in loads:
        load.start()

    loads[0].wait()
    names = iota((128, tok_rows), 0)
    first, second = route_ref[0:1, :], route_ref[1:2, :]
    named = (names == first) | (names == second)
    before = iota((tok_rows, tok_rows), 0) < iota((tok_rows, tok_rows), 1)
    earlier = dot(named.astype(bf16), before.astype(bf16))
    for c, chosen in enumerate((first, second)):
        slot = jnp.sum(jnp.where(names == chosen, earlier, 0.0), axis=0, keepdims=True).astype(jnp.int32)
        sender = (slot // per + upper) % 2
        target_ref[c : c + 1, :] = (chosen * 2 + sender) * per + slot % per
    code = jnp.where(named, earlier, -1.0).astype(bf16)

    loads[1].wait()
    for i in range(blocks):
        loads[2 + i].wait()
        rows = slice(i * block, (i + 1) * block)
        widened = tok_ref[rows, :].astype(f32)
        scale = lax.rsqrt(jnp.mean(widened * widened, axis=-1, keepdims=True) + epsilon)
        mine = tok_ref[rows, at].astype(f32)
        normed_ref[rows, :] = ((mine * scale) * gain_ref[:, at]).astype(bf16)

    share = experts // 2
    rows_out = share * per
    stores = []
    for i in range(2):
        owner = (iota((rows_out, 128), 0) // per + i * share == iota((rows_out, 128), 1)).astype(bf16)
        spread = dot(owner, code)
        within = iota((rows_out, tok_rows), 0) % per + half * per
        pick = (spread == within.astype(f32)).astype(bf16)
        out_ref[i * share : (i + 1) * share] = dot(pick, normed_ref[...]).astype(bf16).reshape(share, per, part)
        which = pl.ds(i * share, share)
        stores.append(pltpu.make_async_copy(out_ref.at[which], out_hbm.at[which], store_sem.at[i]))
        stores[-1].start()
    for store in stores:
        store.wait()


def half_kernel(me_ref, a_ref, wg_ref, wu_ref, vg_ref, vu_ref, *out_refs):
    part = a_ref.shape[1]
    units = wg_ref.shape[1]
    rows = out_refs[0].shape[0]
    at = pl.ds(pl.multiple_of(me_ref[0] // 2 * part, part), part)
    for i, out_ref in enumerate(out_refs):
        for k, ref in enumerate((wg_ref, wu_ref, vg_ref, vu_ref)):
            out_ref[:, k * units : (k + 1) * units] = dot(a_ref[i * rows : (i + 1) * rows, :], ref[at, :])


def hidden_kernel(me_ref, b_ref, wg_ref, wu_ref, vg_ref, vu_ref, held_ref, out_ref):
    part = b_ref.shape[1]
    units = wg_ref.shape[1]
    at = pl.ds(pl.multiple_of((1 - me_ref[0] // 2) * part, part), part)
    for k, (g_ref, u_ref) in enumerate(((wg_ref, wu_ref), (vg_ref, vu_ref))):
        cols = 2 * k * units
        gate = held_ref[:, cols : cols + units] + dot(b_ref[...], g_ref[at, :])
        up = held_ref[:, cols + units : cols + 2 * units] + dot(b_ref[...], u_ref[at, :])
        out_ref[:, k * units : (k + 1) * units] = (gate * (1.0 / (1.0 + jnp.exp(-gate))) * up).astype(bf16)


def split_kernel(me_ref, wd_ref, mine_ref, other_ref):
    part = mine_ref.shape[1]
    upper = me_ref[0] // 2
    mine_ref[...] = wd_ref[:, pl.ds(pl.multiple_of(upper * part, part), part)]
    other_ref[...] = wd_ref[:, pl.ds(pl.multiple_of((1 - upper) * part, part), part)]


def down_kernel(turn, a_ref, b_ref, w0_ref, w1_ref, w2_ref, w3_ref, *rest):
    out_hbm, out_ref, sem = rest[-3:]
    units = w0_ref.shape[0]
    ways, experts, per, part = out_ref.shape
    stores = []
    for y in range(ways):
        cols = slice(y * part, (y + 1) * part)
        total = 0.0
        for ref, k, wd_ref in ((a_ref, 0, w0_ref), (a_ref, 1, w1_ref), (b_ref, 0, w2_ref), (b_ref, 1, w3_ref)):
            term = dot(ref[:, k * units : (k + 1) * units], wd_ref[:, cols])
            total = total + term.astype(bf16).astype(f32)
        out_ref[y] = total.astype(bf16).reshape(experts, per, part)
        place = out_hbm.at[pl.ds(turn * experts, experts), y]
        stores.append(pltpu.make_async_copy(out_ref.at[y], place, sem.at[y]))
        stores[-1].start()
    for store in stores:
        store.wait()


def combine_kernel(target_ref, weight_ref, *rest):
    ret_refs, out_ref = rest[:-1], rest[-1]
    rows = ret_refs[0].shape[0]
    tok_rows = out_ref.shape[0]
    total = 0.0
    lanes = iota((tok_rows, rows), 1)
    for c in range(TOPK):
        target = target_ref[:, c : c + 1]
        picked = 0.0
        for k, ref in enumerate(ret_refs):
            pick = (lanes == target - k * rows).astype(bf16)
            picked = picked + dot(pick, ref[...])
        total = total + picked * weight_ref[:, c : c + 1]
    out_ref[...] = total.astype(bf16)


def smem():
    return pl.BlockSpec(memory_space=pltpu.SMEM)


def vmem():
    return pl.BlockSpec(memory_space=pltpu.VMEM)


def call(kernel, out_shape, args, flops, scratch=(), mib=48):
    outs = out_shape if isinstance(out_shape, (tuple, list)) else (out_shape,)
    moved = sum(a.size * a.dtype.itemsize for a in args) + sum(
        math.prod(o.shape) * o.dtype.itemsize for o in outs
    )
    return pl.pallas_call(
        kernel,
        out_shape=out_shape,
        in_specs=[smem() if a.size == 1 else vmem() for a in args],
        out_specs=jax.tree.map(lambda _: vmem(), out_shape),
        scratch_shapes=list(scratch),
        compiler_params=params(mib),
        cost_estimate=pl.CostEstimate(flops=flops, transcendentals=0, bytes_accessed=moved),
    )(*args)


def shape(*dims, dtype=bf16):
    return jax.ShapeDtypeStruct(dims, dtype)


def inner(
    query_latent,
    key_latent,
    rope_key,
    query_gain,
    key_gain,
    w_query,
    w_query_rope,
    w_key,
    w_value,
    w_out,
    tokens_b,
    ffn_gain,
    route_expert,
    route_weight,
    w_gate,
    w_up,
    w_down,
):
    tp = lax.axis_size(TP)
    experts = lax.axis_size(EP)
    me = lax.axis_index(TP).astype(jnp.int32).reshape(1)

    def ahead(k, n=tp):
        return [(i, (i + k) % n) for i in range(n)]

    def across(k):
        return [(i, i ^ k) for i in range(tp)]

    far_gate = lax.ppermute(w_gate[0], TP, across(1))
    far_up = lax.ppermute(w_up[0], TP, across(1))

    tok_b, width = tokens_b.shape
    per = TOPK * tok_b // experts // 2
    part = width // 2
    rows = experts * per
    units = w_gate.shape[2]
    far = pl.BlockSpec(memory_space=pltpu.HBM)
    target, outgoing = pl.pallas_call(
        prep_kernel,
        out_shape=[shape(TOPK, tok_b, dtype=jnp.int32), shape(experts, per, part)],
        in_specs=[smem(), far, far, far],
        out_specs=[vmem(), far],
        scratch_shapes=[
            pltpu.VMEM((tok_b, width), bf16),
            pltpu.VMEM((1, width), f32),
            pltpu.VMEM((TOPK, tok_b), jnp.int32),
            pltpu.VMEM((tok_b, part), bf16),
            pltpu.VMEM((experts, per, part), bf16),
            pltpu.SemaphoreType.DMA((6,)),
            pltpu.SemaphoreType.DMA((2,)),
        ],
        compiler_params=params(48),
        cost_estimate=pl.CostEstimate(flops=6 * 10**8, transcendentals=0, bytes_accessed=4 * 10**6),
        name="prep",
    )(
        me,
        pltpu.with_memory_space_constraint(tokens_b, pltpu.HBM),
        pltpu.with_memory_space_constraint(ffn_gain.reshape(1, -1), pltpu.HBM),
        pltpu.with_memory_space_constraint(route_expert.T, pltpu.HBM),
    )
    arrived = lax.all_to_all(outgoing, EP, 0, 0, tiled=True)
    arrived = arrived.reshape(rows, part)

    mine, other = call(split_kernel, [shape(units, part)] * 2, (me, w_down[0]), 10**6)
    down3 = lax.ppermute(other, TP, across(3))
    down1 = lax.ppermute(mine, TP, across(1))
    down2 = lax.ppermute(down3, TP, across(1))
    down = (mine, down1, down3, down2)

    tok_a = query_latent.shape[0]
    heads = w_query.shape[1] // NOPE
    cosine, sine = rotary_lanes(tok_a)
    rank = key_latent.shape[1]
    sent = tok_a + tok_a * ROPE // rank
    depth = lax.axis_size("z")
    send = call(latent_kernel, shape(sent, rank), (key_latent, rope_key, key_gain.reshape(1, -1), cosine, sine), 10**7)
    wide = lax.axis_size("x")
    row = [send]
    for k in range(1, wide):
        row.append(lax.ppermute(send, "x", ahead(k, wide)))
    row = call(join_kernel, shape(wide, sent, rank), tuple(row), 10**6)
    queries = call(
        query_kernel,
        shape(heads, tok_a, NOPE + 2 * ROPE),
        (query_latent, query_gain.reshape(1, -1), w_query, w_query_rope, cosine, sine),
        10**8,
    )

    halves = 2
    few = rows // halves
    weights = (w_gate[0], w_up[0], far_gate, far_up)
    joined = []
    for i in range(halves):
        joined.append(lax.ppermute(arrived[i * few : (i + 1) * few], TP, across(3)))
    held = call(
        half_kernel, [shape(few, 4 * units, dtype=f32)] * halves, (me, arrived, *weights), 8 * rows * part * units
    )
    result = ()
    for i in range(halves):
        hidden = call(hidden_kernel, shape(few, 2 * units), (me, joined[i], *weights, held[i]), 8 * few * part * units)
        far_hidden = lax.ppermute(hidden, TP, across(3))
        operands = (hidden, far_hidden, *down)
        result = (
            pl.pallas_call(
                functools.partial(down_kernel, i),
                out_shape=shape(experts, 2, per, part // 2),
                in_specs=[vmem()] * len(operands) + [far] * len(result),
                out_specs=far,
                scratch_shapes=[
                    pltpu.VMEM((2, experts // halves, per, part // 2), bf16),
                    pltpu.SemaphoreType.DMA((2,)),
                ],
                input_output_aliases={len(operands): 0} if result else {},
                compiler_params=params(48),
                cost_estimate=pl.CostEstimate(
                    flops=8 * few * units * part, transcendentals=0, bytes_accessed=4 * 10**6
                ),
                name="down",
            )(*operands, *result),
        )
    result = result[0]

    near = [row]
    up, low = row, row
    for k in range(1, depth // 2 + 1):
        up = lax.ppermute(up, "z", ahead(1, depth))
        near.append(up)
        if 2 * k < depth:
            low = lax.ppermute(low, "z", ahead(depth - 1, depth))
            near.append(low)
    pieces = []
    for piece in near:
        pieces += [piece, lax.ppermute(piece, "c", [(0, 1), (1, 0)])]

    share = shape(tok_a // tp, w_out.shape[1])
    count = len(pieces)
    shares = pl.pallas_call(
        functools.partial(attend_kernel, count),
        out_shape=[share] * tp,
        in_specs=[smem()] + [vmem()] * 4 + [far] * count,
        out_specs=[vmem()] * tp,
        scratch_shapes=[
            pltpu.VMEM((count, *pieces[0].shape), bf16),
            pltpu.VMEM((tok_a, w_out.shape[1]), bf16),
            pltpu.VMEM((heads, tok_a), f32),
            pltpu.VMEM((heads, tok_a), f32),
            pltpu.VMEM((heads, VDIM, tok_a), f32),
            pltpu.SemaphoreType.DMA((count,)),
        ],
        compiler_params=params(48),
        cost_estimate=pl.CostEstimate(flops=6 * 10**9, transcendentals=0, bytes_accessed=8 * 10**6),
        name="attend",
    )(me, queries, w_key, w_value, w_out, *pieces)
    held = [shares[0]]
    for k in range(1, tp):
        held.append(lax.ppermute(shares[k], TP, ahead(k)))
    mixer_out = sum(s.astype(f32) for s in held).astype(bf16)

    returned = lax.all_to_all(result.reshape(2 * experts, per, part // 2), (*EP, "yl"), 0, 0, tiled=True)
    moe_out = call(
        combine_kernel,
        shape(tok_b, part // 2),
        (target.T, route_weight, returned.reshape(2 * rows, part // 2)),
        4 * tok_b * 2 * rows * part // 2,
    )
    return (mixer_out, moe_out)


def spec(*dims):
    spread = {"ep": EP, "tp": TP, "both": EP + TP}
    return P(*(spread.get(d) for d in dims))


def solution(mesh):
    ep, tp = mesh.devices.shape
    fine = Mesh(mesh.devices.reshape(ep // 8, 4, 2, tp // 2, 2), EP + TP)
    in_specs = (
        spec("ep", None),
        spec("ep", None),
        spec("ep", None),
        spec(),
        spec(),
        spec(None, "tp"),
        spec(None, "tp"),
        spec(None, "tp"),
        spec(None, "tp"),
        spec("tp", None),
        spec("ep", None),
        spec(),
        spec("ep", None),
        spec("ep", None),
        spec("ep", None, "tp"),
        spec("ep", None, "tp"),
        spec("ep", "tp", None),
    )
    out_specs = (spec("both", None), spec("ep", "tp"))
    return jax.shard_map(inner, mesh=fine, in_specs=in_specs, out_specs=out_specs, check_vma=False)
```
